32 devices in a mesh: fs: 8 (over z, y), tp: 4 (over x, core).
Axes of the slice: x: 2, y: 2, z: 4, core: 2. Of those that a mesh axis runs over, the one named last changes fastest.
Arguments:
- cotangent: bfloat16 [5120, 1024], P('fs', 'tp'), may hold values from -6 to 6
- inputs: bfloat16 [5120, 1024], P('fs', 'tp'), may hold values from -6 to 6
- pre_act: bfloat16 [5120, 2112], P('fs'), may hold values from -6 to 6
- w_up: bfloat16 [2112, 1024], P('fs', 'tp'), may hold values from -0.1875 to 0.1875
- w_down: bfloat16 [2112, 1024], P('fs', 'tp'), may hold values from -0.125 to 0.125
Outputs:
- grad_input: bfloat16 [5120, 1024], P('fs', 'tp')
- grad_up: float32 [2112, 1024], P('fs', 'tp')
The draws below stay inside these ranges and needn't reach their ends.
All inputs are finite; a program needn't handle non-finite values.
Results may differ from the reference program's by a relative error of at most 0.0049.
Values may be sent and summed in bfloat16 or wider, within the bound.
No kernel may reach another device: no remote copies, remote signals or barrier semaphores. Data moves between devices by JAX's collectives and lax.ppermute only.
A program may use at most 64 MiB of HBM per device.

```python
import jax
import jax.numpy as jnp
from jax import lax

D = 1024
FF = 2112
TOKENS = 5120


def strengthened(drawn, stream_key, source, target, shards_of, factor):
    owner, partner = [(jnp.arange(drawn.shape[position]) // (drawn.shape[position] // shards_of)).reshape([-1 if axis == position else 1 for axis in range(drawn.ndim)]) for position in (source, target)]
    chosen = jax.random.permutation(stream_key, shards_of)[partner]
    strong = (owner == chosen) | (owner == (partner + shards_of // 2) % shards_of)
    return jnp.where(strong, factor * drawn, drawn)


def block_levels(stream_key, shape, pieces, low, largest):
    gain, own = 1.0, jax.random.fold_in(stream_key, 6)
    for dim, parts in pieces:
        draws = jnp.exp(jax.random.uniform(jax.random.fold_in(own, dim), (parts,), jnp.float32, low / len(pieces), largest / len(pieces)))
        gain = gain * jnp.repeat(draws, shape[dim] // parts).reshape([-1 if axis == dim else 1 for axis in range(len(shape))])
    return gain


def bell_draw(key, extent, scale, limit, pieces=(), kind=jnp.bfloat16):
    level = block_levels(key, extent, pieces, -0.22, 0.18) if pieces else 1.0
    result = jax.random.normal(key, extent, jnp.float32) * scale * level
    return jnp.minimum(jnp.maximum(result, -limit), limit).astype(kind)


def gaussian_with(key, shape, deviation, reach, pieces, heavy, kind=jnp.bfloat16):
    drawn = deviation * jax.random.normal(key, shape, jnp.float32)
    if pieces:
        drawn = drawn * block_levels(key, shape, pieces, -0.22, 0.18)
    return jnp.clip(strengthened(drawn, jax.random.fold_in(key, 3), *heavy), -reach, reach).astype(kind)


def setup_inputs(seed: int = 0) -> dict:
    key_of = jax.random.split(jax.random.key(seed), 6)
    return {
        "cotangent": bell_draw(key_of[0], (TOKENS, D), 1.0, 6.0, ((0, 8), (1, 4))),
        "inputs": bell_draw(key_of[1], (TOKENS, D), 1.0, 6.0, ((0, 8), (1, 4))),
        "pre_act": gaussian_with(key_of[2], (TOKENS, FF), 1.0, 6.0, ((0, 8),), (0, 1, 8, 2.0)),
        "w_up": bell_draw(key_of[3], (FF, D), D ** -0.5, 0.1875, ((0, 8), (1, 4))),
        "w_down": bell_draw(key_of[4], (FF, D), FF ** -0.5, 0.125, ((0, 8), (1, 4))),
    }


def reference(cotangent, inputs, pre_act, w_up, w_down):
    grad_hidden = lax.dot_general(cotangent, w_down, (((1,), (1,)), ((), ())), preferred_element_type=jnp.float32)
    grad_pre = (2.0 * grad_hidden * jnp.maximum(pre_act.astype(jnp.float32), 0.0)).astype(jnp.bfloat16)
    grad_input = jnp.dot(grad_pre, w_up, preferred_element_type=jnp.float32).astype(jnp.bfloat16)
    summed = lax.dot_general(grad_pre, inputs, (((0,), (0,)), ((), ())), preferred_element_type=jnp.float32)
    grad_up = summed / jnp.sqrt(jnp.float32(TOKENS))
    return (grad_input, grad_up)
```

```python
import math

import jax
import jax.numpy as jnp
from jax import lax
from jax.sharding import PartitionSpec as P

BF, F32 = jnp.bfloat16, jnp.float32


def radices(n):
    out, stride, p = [], 1, 2
    while n > 1:
        while n % p:
            p += 1
        out.append((stride, p))
        stride, n = stride * p, n // p
    return out


class Axis:
    def __init__(self, name):
        self.name, self.size = name, lax.axis_size(name)
        self.digits = radices(self.size)
        self.index = lax.axis_index(name)

    def add(self, i, k, sign=1):
        out = 0
        for stride, r in self.digits:
            out = out + ((i // stride % r + sign * (k // stride % r)) % r) * stride
        return out

    def neg(self, k):
        return self.add(0, k, -1)

    def send(self, v, k):
        return lax.ppermute(v, self.name, [(i, self.add(i, k)) for i in range(self.size)])

    def parent(self, k):
        for stride, r in self.digits:
            part = k // stride % r * stride
            if part:
                return k - part, part
        return None

    def depth(self, k):
        return sum(1 for stride, r in self.digits if k // stride % r)

    def gather(self, v):
        blocks = {0: v}
        for k in sorted(range(1, self.size), key=self.depth):
            p, part = self.parent(k)
            blocks[k] = self.send(blocks[p], part)
        return blocks

    def reduce(self, parts):
        total = dict(parts)
        for k in sorted(range(1, self.size), key=self.depth, reverse=True):
            p, part = self.parent(k)
            total[p] = total[p] + self.send(total[k].astype(BF), part).astype(F32)
        return total[0]


def dot(a, b, ca, cb):
    return lax.dot_general(a, b, (((ca,), (cb,)), ((), ())), preferred_element_type=F32)


def local(cotangent, inputs, pre_act, w_up, w_down):
    fs, tp = Axis("fs"), Axis("tp")
    rows, width = w_down.shape
    tokens = cotangent.shape[0]
    q = -(-rows // (tp.size * 8)) * 8
    starts = [min(j * q, rows - q) for j in range(tp.size)]
    start_of = jnp.array(starts, jnp.int32)
    skip_of = jnp.array([j * q - starts[j] for j in range(tp.size)], jnp.int32)

    def piece(w, k):
        j = tp.add(tp.index, k)
        cut = lax.dynamic_slice(w, (start_of[j], 0), (q, width))
        return jnp.where(lax.broadcasted_iota(jnp.int32, (q, width), 0) >= skip_of[j], cut, jnp.zeros_like(cut))

    got = []
    for k in range(tp.size):
        both = jnp.concatenate([piece(w_down, k), piece(w_up, k)], axis=0)
        got.append(tp.send(both, k) if k else both)
    down = jnp.concatenate([g[:q] for g in got], axis=1)
    up = jnp.concatenate([g[q:] for g in got], axis=1)
    cots = tp.gather(cotangent)
    cot = jnp.concatenate([cots[k] for k in range(tp.size)], axis=1)
    inps = tp.gather(inputs)
    inp = jnp.concatenate([inps[k] for k in range(tp.size)], axis=1)

    downs = fs.gather(down)
    ups = fs.gather(up)
    pre_t = pre_act.T
    hidden, shares = {}, {}
    for k in range(fs.size):
        source = fs.add(fs.index, k, -1)
        act = lax.dynamic_slice(pre_t, (source * rows + start_of[tp.index], 0), (q, tokens))
        grad_hidden = dot(downs[k], cot, 1, 1)
        hidden[k] = (2.0 * grad_hidden * jnp.maximum(act.astype(F32), 0.0)).astype(BF)
        shares[fs.neg(k)] = dot(hidden[k], inp, 1, 0)
    grad_rows = fs.reduce(shares)

    every = range(fs.size)
    part = dot(
        jnp.concatenate([hidden[k] for k in every], axis=0),
        jnp.concatenate([ups[k] for k in every], axis=0), 0, 0,
    )
    cut = lambda v, k: v[:, k * width : (k + 1) * width]
    grad_input = tp.reduce({tp.neg(k): cut(part, k) for k in range(tp.size)}).astype(BF)

    scaled = grad_rows / jnp.sqrt(jnp.float32(tokens * fs.size))
    mine = {0: cut(scaled, 0)}
    for k in range(1, tp.size):
        mine[k] = tp.send(cut(scaled, k), tp.neg(k))
    pieces = jnp.stack([mine[k] for k in range(tp.size)])
    out = []
    for j in range(tp.size):
        keep = min(q, rows - j * q)
        if keep > 0:
            k = tp.add(j, tp.index, -1)
            out.append(lax.dynamic_index_in_dim(pieces, k, 0, keepdims=False)[q - keep :])
    return grad_input, jnp.concatenate(out, axis=0)


def solution(mesh):
    return jax.shard_map(
        local,
        mesh=mesh,
        in_specs=(P("fs", "tp"), P("fs", "tp"), P("fs", None), P("fs", "tp"), P("fs", "tp")),
        out_specs=(P("fs", "tp"), P("fs", "tp")),
        check_vma=False,
    )
```
